32 devices in a mesh: grp: 2 (over y), fs: 4 (over z), tp: 4 (over x, core).
Axes of the slice: x: 2, y: 2, z: 4, core: 2. Of those that a mesh axis runs over, the one named last changes fastest.
Arguments:
- tokens: bfloat16 [512, 2048], P(('grp', 'fs')), parts along dimension 0, may hold values from -6 to 6
- routes: int32 [512, 2], P(('grp', 'fs')), parts along dimension 0, may hold values from 0 to 3, as said below
- route_logits: float32 [512, 2], P(('grp', 'fs')), parts along dimension 0, may hold values from -8 to 8
- gain: float32 [2048], P('fs'), may hold values from 0.1 to 1.9
- w_gate: float32 [4, 2048, 7168], P(None, 'fs', 'tp'), may hold values from -0.125 to 0.125
- w_up: float32 [4, 2048, 7168], P(None, 'fs', 'tp'), may hold values from -0.125 to 0.125
- w_down: float32 [4, 7168, 2048], P(None, 'fs', 'tp'), may hold values from -0.0625 to 0.0625
Outputs:
- gate_served: bfloat16 [8, 2048, 7168], P(('grp', 'tp'), None, 'fs'), parts along dimension 0
- up_served: bfloat16 [8, 2048, 7168], P(('grp', 'tp'), None, 'fs'), parts along dimension 0
- down_served: bfloat16 [8, 7168, 2048], P(('grp', 'tp'), 'fs'), parts along dimension 0
- mixed: bfloat16 [512, 2048], P(('grp', 'fs'), 'tp'), parts along dimension 0
The draws below stay inside these ranges and needn't reach their ends.
There are 2 independent parts, one for each index of `grp`. The reference program is written for one: setup_inputs(seed, part) draws one part's arguments, and reference() takes and returns one part's arrays. A program takes and returns all parts, laid end to end along the dimension named above; an argument that names none is the same for every part. Nothing has to cross between parts.
Inputs may be any that keep to these rules, and one draw needn't show every extreme that they name: `routes`: each row names 2 different experts; every expert is named by some row.
All inputs are finite; a program needn't handle non-finite values.
Results may differ from the reference program's by a relative error of at most 0.0085.
Values may be sent and summed in bfloat16 or wider, within the bound.
A program may use at most 192 MiB of HBM per device.

```python
import jax
import jax.numpy as jnp
from jax import lax

D = 2048
FF = 7168
EXPERTS = 4
TOP = 2
TOKENS = 256


def draw_routes(key, part):
    key_hot = jax.random.fold_in(key, 101)
    key_pick = jax.random.fold_in(key, 102)
    key_other = jax.random.fold_in(key, 103)
    key_second = jax.random.fold_in(key, 104)
    hot_expert = jax.random.randint(key_hot, (), 0, EXPERTS, dtype=jnp.int32)
    chooser = jax.random.randint(key_pick, (TOKENS,), 0, 8, dtype=jnp.int32)
    other_offset = jax.random.randint(key_other, (TOKENS,), 0, EXPERTS - 1, dtype=jnp.int32)
    other_expert = (hot_expert + 1 + other_offset) % EXPERTS
    first_col = jnp.where(chooser < 7, hot_expert, other_expert).astype(jnp.int32)
    second_offset = jax.random.randint(key_second, (TOKENS,), 0, EXPERTS - 1, dtype=jnp.int32)
    second_col = ((first_col + 1 + second_offset) % EXPERTS).astype(jnp.int32)
    row_index = jnp.arange(TOKENS, dtype=jnp.int32)
    first_col = jnp.where(row_index < EXPERTS, row_index, first_col)
    second_col = jnp.where(row_index < EXPERTS, (row_index + 1) % EXPERTS, second_col)
    return jnp.stack([first_col, second_col], axis=1).astype(jnp.int32)


def steps_of(stream_key, extent, pieces, low, largest):
    def one(axis_at, shards_of):
        draws = jax.random.uniform(jax.random.fold_in(jax.random.fold_in(stream_key, 6), axis_at), (shards_of,), jnp.float32, low / len(pieces), largest / len(pieces))
        return jnp.repeat(jnp.exp(draws), extent[axis_at] // shards_of).reshape((-1,) + (1,) * (len(extent) - axis_at - 1))

    level = one(*pieces[0])
    for cut in pieces[1:]:
        level = level * one(*cut)
    return level


def gaussian(stream_key, dims, width, reach, split=(), held_as=jnp.bfloat16):
    array = jax.random.normal(stream_key, dims, jnp.float32) * width
    if len(split) > 0:
        array = steps_of(stream_key, dims, split, -0.22, 0.18) * array
    return jnp.clip(array, min=-reach, max=reach).astype(held_as)


def setup_inputs(seed: int = 0, part: int = 0) -> dict:
    splits = jax.random.split(jax.random.key(seed), 8)
    own_keys = jax.random.split(jax.random.fold_in(splits[7], part), 8)
    tokens = gaussian(own_keys[0], (TOKENS, D), 1.0, 6.0, ((0, 4),))
    routes = draw_routes(jax.random.fold_in(jax.random.fold_in(splits[7], part), 71), part)
    route_logits = gaussian(own_keys[2], (TOKENS, TOP), 1.5, 8.0, ((0, 4),), jnp.float32)
    gain = jnp.clip(1.0 + 0.18 * jax.random.normal(splits[3], (D,), jnp.float32), 0.1, 1.9)
    w_gate = gaussian(splits[4], (EXPERTS, D, FF), D ** -0.5, 0.125, ((1, 4), (2, 4)), jnp.float32)
    w_up = gaussian(splits[5], (EXPERTS, D, FF), D ** -0.5, 0.125, ((1, 4), (2, 4)), jnp.float32)
    w_down = gaussian(splits[6], (EXPERTS, FF, D), FF ** -0.5, 0.0625, ((1, 4), (2, 4)), jnp.float32)
    return {"tokens": tokens, "routes": routes, "route_logits": route_logits, "gain": gain, "w_gate": w_gate, "w_up": w_up, "w_down": w_down}


def reference(tokens, routes, route_logits, gain, w_gate, w_up, w_down):
    values = tokens.astype(jnp.float32)
    mean_square = lax.optimization_barrier(jnp.mean(values * values, axis=-1, keepdims=True))
    normed = (values * lax.rsqrt(mean_square + 1e-06)).astype(jnp.bfloat16)
    first = jax.nn.sigmoid(route_logits[:, 0] - route_logits[:, 1])
    second = jax.nn.sigmoid(route_logits[:, 1] - route_logits[:, 0])
    gate_cast = (w_gate * gain[None, :, None]).astype(jnp.bfloat16)
    up_cast = (w_up * gain[None, :, None]).astype(jnp.bfloat16)
    down_cast = w_down.astype(jnp.bfloat16)
    total = jnp.zeros((tokens.shape[0], w_down.shape[2]), jnp.float32)
    for expert in range(EXPERTS):
        weight_col = first * (routes[:, 0] == expert).astype(jnp.float32)
        weight_col = weight_col + second * (routes[:, 1] == expert).astype(jnp.float32)
        weight_col = weight_col.astype(jnp.bfloat16)
        gate_act = jnp.dot(normed, gate_cast[expert], preferred_element_type=jnp.float32)
        up_act = jnp.dot(normed, up_cast[expert], preferred_element_type=jnp.float32)
        hidden = (jax.nn.silu(gate_act) * up_act * weight_col[:, None].astype(jnp.float32)).astype(jnp.bfloat16)
        total = total + jnp.dot(hidden, down_cast[expert], preferred_element_type=jnp.float32)
    return (gate_cast, up_cast, down_cast, total.astype(jnp.bfloat16))
```

```python
import functools

import jax
import jax.numpy as jnp
from jax import lax
from jax.experimental import pallas as pl
from jax.experimental.pallas import tpu as pltpu
from jax.sharding import PartitionSpec as P

BF16 = jnp.bfloat16
F32 = jnp.float32
CHUNKS = 4
DOWN_CHUNKS = 4
LOADS = 4


def move_kernel(
    groups, n, gain_ref, wg_ref, wu_ref, wd_ref, og_ref, ou_ref, od_ref,
    wide, wide_d, stage, extra, relay, stage_d,
    load_sem, s1s, s1r, xs, xr, zs, zr, ys, yr, ds, dr,
):
    g, f, t = lax.axis_index("grp"), lax.axis_index("fs"), lax.axis_index("tp")
    rows = wg_ref.shape[1]
    half = rows // groups
    ch = half // CHUNKS
    hidden, width = wd_ref.shape[1:]
    dh = hidden // DOWN_CHUNKS
    weights, outs = (wg_ref, wu_ref), (og_ref, ou_ref)
    items = 2 * CHUNKS

    mate = t + 1 - 2 * lax.rem(t, 2)
    peers = (t, mate, lax.rem(t + 2, n), lax.rem(mate + 2, n))
    home = f == t

    def remote(src, dst, ssem, rsem, where):
        return pltpu.make_async_remote_copy(
            src_ref=src, dst_ref=dst, send_sem=ssem, recv_sem=rsem,
            device_id=where, device_id_type=pl.DeviceIdType.MESH,
        )

    barrier = pltpu.get_barrier_semaphore()
    for k in (1, 2, 3):
        pl.semaphore_signal(barrier, inc=1, device_id=(g, f, peers[k]), device_id_type=pl.DeviceIdType.MESH)
    for d in range(1, n):
        pl.semaphore_signal(barrier, inc=1, device_id=(g, lax.rem(f + d, n), t), device_id_type=pl.DeviceIdType.MESH)
    pl.semaphore_signal(barrier, inc=1, device_id=(1 - g, f, t), device_id_type=pl.DeviceIdType.MESH)
    pl.semaphore_wait(barrier, 2 * n - 1)

    def own_row(c):
        return pl.multiple_of(g * half + c * ch, ch)

    def other_row(c):
        return pl.multiple_of((1 - g) * half + c * ch, ch)

    def at_rows(u, source, row):
        return outs[u].at[pl.ds(pl.multiple_of(source * rows + row, ch), ch), :]

    def first(k, u, c):
        return remote(stage.at[k, u, c], relay.at[k - 1, u, c], s1s.at[k, u, c], s1r.at[k, u, c], (g, f, peers[k]))

    def first_home(k, u, c):
        return remote(stage.at[k, u, c], at_rows(u, f, own_row(c)), s1s.at[k, u, c], s1r.at[k, u, c], (g, f, peers[k]))

    def own_home(u, c):
        return pltpu.make_async_copy(stage.at[0, u, c], at_rows(u, f, own_row(c)), s1s.at[0, u, c])

    def extra_home(u, c):
        return pltpu.make_async_copy(extra.at[0, u, c], at_rows(u, f, other_row(c)), xs.at[0, u, c])

    def extra_mate(u, c):
        return remote(extra.at[1, u, c], at_rows(u, f, other_row(c)), xs.at[1, u, c], xr.at[u, c], (g, f, mate))

    def layer(k, u, c):
        src = stage.at[0, u, c] if k == 0 else relay.at[k - 1, u, c]
        return remote(src, at_rows(u, f, own_row(c)), zs.at[k, u, c], zr.at[f, u, c], (g, peers[k], t))

    def layer_in(source, u, c):
        piece = at_rows(u, source, own_row(c))
        return remote(piece, piece, zs.at[0, u, c], zr.at[source, u, c], (1 - g, f, t))

    def across(source, u, c):
        piece = at_rows(u, source, own_row(c))
        return remote(piece, piece, ys.at[source, u, c], yr.at[source, u, c], (1 - g, f, t))

    def down(k, c):
        src = stage_d.at[k, c]
        dst = od_ref.at[pl.ds(c * dh, dh), pl.ds(pl.multiple_of(t * width, 128), width)]
        if k == 0:
            return pltpu.make_async_copy(src, dst, ds.at[0, c])
        return remote(src, dst, ds.at[k, c], dr.at[k, c], (g, f, peers[k]))

    order = (2, 0, 3, 1)

    def load(u, k, row, slot):
        return pltpu.make_async_copy(weights[u].at[peers[k], pl.ds(row, ch), :], wide.at[slot], load_sem.at[slot])

    def load_d(k, c, slot):
        return pltpu.make_async_copy(wd_ref.at[peers[k], pl.ds(c * dh, dh), :], wide_d.at[slot], load_sem.at[LOADS + slot])

    def fold(slot, row, dst):
        scale = gain_ref[pl.ds(row, ch), :]
        dst[...] = (wide[slot] * scale).astype(BF16)

    for j, k in enumerate(order):
        load(0, k, own_row(0), j).start()
    for u in range(2):
        def trip(c, _, u=u):
            for j, k in enumerate(order):
                load(u, k, own_row(c), j).wait()
                fold(j, own_row(c), stage.at[k, u, c])

                @pl.when(c < CHUNKS - 1)
                def _():
                    load(u, k, own_row(c + 1), j).start()

                if u == 0:
                    @pl.when(c == CHUNKS - 1)
                    def _():
                        load(1, k, own_row(0), j).start()

                if k == 0:
                    @pl.when(home)
                    def _():
                        own_home(u, c).start()

                    @pl.when(jnp.logical_not(home))
                    def _():
                        layer(0, u, c).start()
                else:
                    @pl.when(home)
                    def _():
                        first_home(k, u, c).start()

                    @pl.when(jnp.logical_not(home))
                    def _():
                        first(k, u, c).start()
            return 0

        lax.fori_loop(0, CHUNKS, trip, 0)

    for j, k in enumerate(order):
        load_d(k, 0, j).start()

    def trip_d(c, _):
        for j, k in enumerate(order):
            load_d(k, c, j).wait()
            stage_d[k, c] = wide_d[j].astype(BF16)

            @pl.when(c < DOWN_CHUNKS - 1)
            def _():
                load_d(k, c + 1, j).start()

            down(k, c).start()
        return 0

    lax.fori_loop(0, DOWN_CHUNKS, trip_d, 0)

    @pl.when(home)
    def _():
        for u in range(2):
            def trip_x(c, _, u=u):
                for k in (0, 1):
                    copy = load(u, k, other_row(c), k)
                    copy.start()
                    copy.wait()
                    fold(k, other_row(c), extra.at[k, u, c])
                    (extra_home if k == 0 else extra_mate)(u, c).start()
                return 0

            lax.fori_loop(0, CHUNKS, trip_x, 0)

    def forward_z(k, u, c):
        away = peers[k] != f

        @pl.when(away)
        def _():
            first(k, u, c).wait_recv()
            layer(k, u, c).start()

        @pl.when(jnp.logical_not(away))
        def _():
            first_home(k, u, c).wait_recv()
            if k >= 2:
                across(f, u, c).start()

    def forward_y(d, u, c):
        for sign in (1, -1):
            source = f + sign * d

            @pl.when((source >= 0) & (source < n))
            def _():
                layer_in(source, u, c).wait_recv()
                across(source, u, c).start()

    lag = min(2, items)

    def at_item(fn, i):
        u, c = i // CHUNKS, lax.rem(i, CHUNKS)
        for v in range(2):
            @pl.when(u == v)
            def _():
                fn(v, c)

    def trip_f(i, _):
        def z_part(u, c):
            for k in (1, 2, 3):
                forward_z(k, u, c)

        at_item(z_part, i)

        @pl.when(i >= lag)
        def _():
            at_item(functools.partial(forward_y, 1), i - lag)

        return 0

    lax.fori_loop(0, items, trip_f, 0)

    def trip_t(i, _):
        at_item(functools.partial(forward_y, 1), i)
        return 0

    lax.fori_loop(items - lag, items, trip_t, 0)

    def trip_r(i, _):
        at_item(functools.partial(forward_y, 2), i)
        at_item(functools.partial(forward_y, 3), i)
        return 0

    lax.fori_loop(0, items, trip_r, 0)

    for u in range(2):
        def trip_w(c, _, u=u):
            @pl.when(home)
            def _():
                own_home(u, c).wait()
                extra_home(u, c).wait()
                extra_mate(u, c).wait_send()

            @pl.when(jnp.logical_not(home))
            def _():
                layer(0, u, c).wait_send()

            @pl.when(f == mate)
            def _():
                extra_mate(u, c).wait_recv()

            for k in (1, 2, 3):
                first(k, u, c).wait_send()

                @pl.when(peers[k] != f)
                def _():
                    layer(k, u, c).wait_send()

                if k >= 2:
                    @pl.when(peers[k] == f)
                    def _():
                        across(f, u, c).wait()

            for d in range(1, n):
                for sign in (1, -1):
                    source = f + sign * d

                    @pl.when((source >= 0) & (source < n))
                    def _():
                        across(source, u, c).wait()
            return 0

        lax.fori_loop(0, CHUNKS, trip_w, 0)

    def trip_wd(c, _):
        for k in range(n):
            down(k, c).wait()
        return 0

    lax.fori_loop(0, DOWN_CHUNKS, trip_wd, 0)


def move(groups, n, gain, w_gate, w_up, w_down):
    experts, rows, cols = w_gate.shape
    hidden, width = w_down.shape[1:]
    ch = rows // groups // CHUNKS
    dh = hidden // DOWN_CHUNKS
    dma = pltpu.SemaphoreType.DMA
    hbm = pl.BlockSpec(memory_space=pl.ANY)
    return pl.pallas_call(
        functools.partial(move_kernel, groups, n),
        out_shape=(
            jax.ShapeDtypeStruct((rows * n, cols), BF16),
            jax.ShapeDtypeStruct((rows * n, cols), BF16),
            jax.ShapeDtypeStruct((hidden, width * n), BF16),
        ),
        in_specs=[pl.BlockSpec(memory_space=pltpu.VMEM), hbm, hbm, hbm],
        out_specs=(hbm, hbm, hbm),
        scratch_shapes=[
            pltpu.VMEM((LOADS, ch, cols), F32),
            pltpu.VMEM((LOADS, dh, width), F32),
            pltpu.VMEM((n, 2, CHUNKS, ch, cols), BF16),
            pltpu.VMEM((2, 2, CHUNKS, ch, cols), BF16),
            pltpu.VMEM((n - 1, 2, CHUNKS, ch, cols), BF16),
            pltpu.VMEM((n, DOWN_CHUNKS, dh, width), BF16),
            dma((2 * LOADS,)),
            dma((n, 2, CHUNKS)),
            dma((n, 2, CHUNKS)),
            dma((2, 2, CHUNKS)),
            dma((2, CHUNKS)),
            dma((n, 2, CHUNKS)),
            dma((n, 2, CHUNKS)),
            dma((n, 2, CHUNKS)),
            dma((n, 2, CHUNKS)),
            dma((n, DOWN_CHUNKS)),
            dma((n, DOWN_CHUNKS)),
        ],
        name="move_weights",
        compiler_params=pltpu.CompilerParams(
            collective_id=0, has_side_effects=True, vmem_limit_bytes=56 << 20
        ),
    )(gain.reshape(rows, 1), w_gate, w_up, w_down)


def hand_over(mesh, gain, w_gate, w_up, w_down):
    groups, n, tp = mesh.shape["grp"], mesh.shape["fs"], mesh.shape["tp"]
    rows, cols = w_gate.shape[1:]
    hidden, width = w_down.shape[1:]
    direct = (
        groups == 2 and n == 4 and tp == 4 and w_gate.shape[0] == tp
        and cols % 128 == 0 and width % 128 == 0
        and rows % (groups * CHUNKS * 16) == 0 and hidden % (DOWN_CHUNKS * 16) == 0
    )
    if direct:
        gate, up, down = move(groups, n, gain, w_gate, w_up, w_down)
        return gate[None], up[None], down[None]
    gate = (w_gate * gain[None, :, None]).astype(BF16)
    up = (w_up * gain[None, :, None]).astype(BF16)
    spread = functools.partial(lax.all_to_all, axis_name="tp", split_axis=0, concat_axis=2, tiled=True)
    gate, up, down = spread(gate), spread(up), spread(w_down.astype(BF16))
    stack = functools.partial(lax.all_to_all, axis_name="fs", split_axis=2, concat_axis=1, tiled=True)
    return stack(gate), stack(up), down


def body(mesh, tokens, routes, route_logits, gain, w_gate, w_up, w_down):
    values = tokens.astype(F32)
    mean_square = jnp.mean(values * values, axis=-1, keepdims=True)
    normed = (values * lax.rsqrt(mean_square + 1e-06)).astype(BF16)
    expert_id = lax.axis_index("tp")
    first = jax.nn.sigmoid(route_logits[:, 0] - route_logits[:, 1])
    second = jax.nn.sigmoid(route_logits[:, 1] - route_logits[:, 0])
    weight_col = first * (routes[:, 0] == expert_id).astype(F32)
    weight_col = (weight_col + second * (routes[:, 1] == expert_id).astype(F32)).astype(BF16)
    piece_rows = lax.all_gather(normed, "fs", axis=0, tiled=True)
    piece_weight = lax.all_gather(weight_col, "fs", axis=0, tiled=True)
    gate_served, up_served, down_served = hand_over(mesh, gain, w_gate, w_up, w_down)
    gate_act = jnp.dot(piece_rows, gate_served[0], preferred_element_type=F32)
    up_act = jnp.dot(piece_rows, up_served[0], preferred_element_type=F32)
    hidden_rows = jax.nn.silu(gate_act) * up_act * piece_weight[:, None].astype(F32)
    hidden = hidden_rows.astype(BF16)
    term = jnp.dot(hidden, down_served[0], preferred_element_type=F32)
    by_feature = lax.psum_scatter(term, "tp", scatter_dimension=1, tiled=True)
    mixed = lax.psum_scatter(by_feature, "fs", scatter_dimension=0, tiled=True)
    return (gate_served, up_served, down_served, mixed.astype(BF16))


def solution(mesh):
    return jax.shard_map(
        functools.partial(body, mesh),
        mesh=mesh,
        in_specs=(
            P(("grp", "fs"), None),
            P(("grp", "fs"), None),
            P(("grp", "fs"), None),
            P("fs"),
            P(None, "fs", "tp"),
            P(None, "fs", "tp"),
            P(None, "fs", "tp"),
        ),
        out_specs=(
            P(("grp", "tp"), None, "fs"),
            P(("grp", "tp"), None, "fs"),
            P(("grp", "tp"), "fs", None),
            P(("grp", "fs"), "tp"),
        ),
        check_vma=False,
    )
```

```python
import functools

import jax
import jax.numpy as jnp
from jax import lax
from jax.experimental import pallas as pl
from jax.experimental.pallas import tpu as pltpu
from jax.sharding import PartitionSpec as P

BF16 = jnp.bfloat16
F32 = jnp.float32
CHUNKS = 4
DOWN_CHUNKS = 4
LAGS = (3, 5, 7)
LOADS = 4


def move_kernel(
    groups, n, gain_ref, wg_ref, wu_ref, wd_ref, og_ref, ou_ref, od_ref,
    wide, wide_d, stage, extra, relay, stage_d,
    load_sem, s1s, s1r, xs, xr, zs, zr, ys, yr, ds, dr,
):
    g, f, t = lax.axis_index("grp"), lax.axis_index("fs"), lax.axis_index("tp")
    rows = wg_ref.shape[1]
    half = rows // groups
    ch = half // CHUNKS
    hidden, width = wd_ref.shape[1:]
    dh = hidden // DOWN_CHUNKS
    weights, outs = (wg_ref, wu_ref), (og_ref, ou_ref)
    items = 2 * CHUNKS

    mate = t + 1 - 2 * lax.rem(t, 2)
    peers = (t, mate, lax.rem(t + 2, n), lax.rem(mate + 2, n))
    home = f == t

    def remote(src, dst, ssem, rsem, where):
        return pltpu.make_async_remote_copy(
            src_ref=src, dst_ref=dst, send_sem=ssem, recv_sem=rsem,
            device_id=where, device_id_type=pl.DeviceIdType.MESH,
        )

    barrier = pltpu.get_barrier_semaphore()
    for k in (1, 2, 3):
        pl.semaphore_signal(barrier, inc=1, device_id=(g, f, peers[k]), device_id_type=pl.DeviceIdType.MESH)
    for d in range(1, n):
        pl.semaphore_signal(barrier, inc=1, device_id=(g, lax.rem(f + d, n), t), device_id_type=pl.DeviceIdType.MESH)
    pl.semaphore_signal(barrier, inc=1, device_id=(1 - g, f, t), device_id_type=pl.DeviceIdType.MESH)
    pl.semaphore_wait(barrier, 2 * n - 1)

    def own_row(c):
        return pl.multiple_of(g * half + c * ch, ch)

    def other_row(c):
        return pl.multiple_of((1 - g) * half + c * ch, ch)

    def at_rows(u, source, row):
        return outs[u].at[pl.ds(pl.multiple_of(source * rows + row, ch), ch), :]

    def first(k, u, c):
        return remote(stage.at[k, u, c], relay.at[k - 1, u, c], s1s.at[k, u, c], s1r.at[k, u, c], (g, f, peers[k]))

    def first_home(k, u, c):
        return remote(stage.at[k, u, c], at_rows(u, f, own_row(c)), s1s.at[k, u, c], s1r.at[k, u, c], (g, f, peers[k]))

    def own_home(u, c):
        return pltpu.make_async_copy(stage.at[0, u, c], at_rows(u, f, own_row(c)), s1s.at[0, u, c])

    def extra_home(u, c):
        return pltpu.make_async_copy(extra.at[0, u, c], at_rows(u, f, other_row(c)), xs.at[0, u, c])

    def extra_mate(u, c):
        return remote(extra.at[1, u, c], at_rows(u, f, other_row(c)), xs.at[1, u, c], xr.at[u, c], (g, f, mate))

    def layer(k, u, c):
        src = stage.at[0, u, c] if k == 0 else relay.at[k - 1, u, c]
        return remote(src, at_rows(u, f, own_row(c)), zs.at[k, u, c], zr.at[f, u, c], (g, peers[k], t))

    def layer_in(source, u, c):
        piece = at_rows(u, source, own_row(c))
        return remote(piece, piece, zs.at[0, u, c], zr.at[source, u, c], (1 - g, f, t))

    def across(source, u, c):
        piece = at_rows(u, source, own_row(c))
        return remote(piece, piece, ys.at[source, u, c], yr.at[source, u, c], (1 - g, f, t))

    def down(k, c):
        src = stage_d.at[k, c]
        dst = od_ref.at[pl.ds(c * dh, dh), pl.ds(pl.multiple_of(t * width, 128), width)]
        if k == 0:
            return pltpu.make_async_copy(src, dst, ds.at[0, c])
        return remote(src, dst, ds.at[k, c], dr.at[k, c], (g, f, peers[k]))

    order = (2, 0, 3, 1)

    def load(u, k, row, slot):
        return pltpu.make_async_copy(weights[u].at[peers[k], pl.ds(row, ch), :], wide.at[slot], load_sem.at[slot])

    def load_d(k, c, slot):
        return pltpu.make_async_copy(wd_ref.at[peers[k], pl.ds(c * dh, dh), :], wide_d.at[slot], load_sem.at[LOADS + slot])

    def fold(slot, row, dst):
        scale = gain_ref[pl.ds(row, ch), :]
        dst[...] = (wide[slot] * scale).astype(BF16)

    for j, k in enumerate(order):
        load(0, k, own_row(0), j).start()
    for u in range(2):
        def trip(c, _, u=u):
            for j, k in enumerate(order):
                load(u, k, own_row(c), j).wait()
                fold(j, own_row(c), stage.at[k, u, c])

                @pl.when(c < CHUNKS - 1)
                def _():
                    load(u, k, own_row(c + 1), j).start()

                if u == 0:
                    @pl.when(c == CHUNKS - 1)
                    def _():
                        load(1, k, own_row(0), j).start()

                if k == 0:
                    @pl.when(home)
                    def _():
                        own_home(u, c).start()

                    @pl.when(jnp.logical_not(home))
                    def _():
                        layer(0, u, c).start()
                else:
                    @pl.when(home)
                    def _():
                        first_home(k, u, c).start()

                    @pl.when(jnp.logical_not(home))
                    def _():
                        first(k, u, c).start()
            return 0

        lax.fori_loop(0, CHUNKS, trip, 0)

    for j, k in enumerate(order):
        load_d(k, 0, j).start()

    def trip_d(c, _):
        for j, k in enumerate(order):
            load_d(k, c, j).wait()
            stage_d[k, c] = wide_d[j].astype(BF16)

            @pl.when(c < DOWN_CHUNKS - 1)
            def _():
                load_d(k, c + 1, j).start()

            down(k, c).start()
        return 0

    lax.fori_loop(0, DOWN_CHUNKS, trip_d, 0)

    @pl.when(home)
    def _():
        for u in range(2):
            def trip_x(c, _, u=u):
                for k in (0, 1):
                    copy = load(u, k, other_row(c), k)
                    copy.start()
                    copy.wait()
                    fold(k, other_row(c), extra.at[k, u, c])
                    (extra_home if k == 0 else extra_mate)(u, c).start()
                return 0

            lax.fori_loop(0, CHUNKS, trip_x, 0)

    def forward_z(k, u, c):
        away = peers[k] != f

        @pl.when(away)
        def _():
            first(k, u, c).wait_recv()
            layer(k, u, c).start()

        @pl.when(jnp.logical_not(away))
        def _():
            first_home(k, u, c).wait_recv()
            if k >= 2:
                across(f, u, c).start()

    def forward_y(d, u, c):
        for sign in (1, -1):
            source = f + sign * d

            @pl.when((source >= 0) & (source < n))
            def _():
                layer_in(source, u, c).wait_recv()
                across(source, u, c).start()

    def at_item(fn, i):
        u, c = i // CHUNKS, lax.rem(i, CHUNKS)
        for v in range(2):
            @pl.when(u == v)
            def _():
                fn(v, c)

    def trip_f(i, _):
        def z_part(u, c):
            for k in (1, 2, 3):
                forward_z(k, u, c)

        @pl.when(i < items)
        def _():
            at_item(z_part, i)

        for d in range(1, n):
            lag = LAGS[d - 1]

            @pl.when((i >= lag) & (i < items + lag))
            def _():
                at_item(functools.partial(forward_y, d), i - lag)

        return 0

    lax.fori_loop(0, items + max(LAGS), trip_f, 0)

    for u in range(2):
        def trip_w(c, _, u=u):
            @pl.when(home)
            def _():
                own_home(u, c).wait()
                extra_home(u, c).wait()
                extra_mate(u, c).wait_send()

            @pl.when(jnp.logical_not(home))
            def _():
                layer(0, u, c).wait_send()

            @pl.when(f == mate)
            def _():
                extra_mate(u, c).wait_recv()

            for k in (1, 2, 3):
                first(k, u, c).wait_send()

                @pl.when(peers[k] != f)
                def _():
                    layer(k, u, c).wait_send()

                if k >= 2:
                    @pl.when(peers[k] == f)
                    def _():
                        across(f, u, c).wait()

            for d in range(1, n):
                for sign in (1, -1):
                    source = f + sign * d

                    @pl.when((source >= 0) & (source < n))
                    def _():
                        across(source, u, c).wait()
            return 0

        lax.fori_loop(0, CHUNKS, trip_w, 0)

    def trip_wd(c, _):
        for k in range(n):
            down(k, c).wait()
        return 0

    lax.fori_loop(0, DOWN_CHUNKS, trip_wd, 0)


def move(groups, n, gain, w_gate, w_up, w_down):
    experts, rows, cols = w_gate.shape
    hidden, width = w_down.shape[1:]
    ch = rows // groups // CHUNKS
    dh = hidden // DOWN_CHUNKS
    dma = pltpu.SemaphoreType.DMA
    hbm = pl.BlockSpec(memory_space=pl.ANY)
    return pl.pallas_call(
        functools.partial(move_kernel, groups, n),
        out_shape=(
            jax.ShapeDtypeStruct((rows * n, cols), BF16),
            jax.ShapeDtypeStruct((rows * n, cols), BF16),
            jax.ShapeDtypeStruct((hidden, width * n), BF16),
        ),
        in_specs=[pl.BlockSpec(memory_space=pltpu.VMEM), hbm, hbm, hbm],
        out_specs=(hbm, hbm, hbm),
        scratch_shapes=[
            pltpu.VMEM((LOADS, ch, cols), F32),
            pltpu.VMEM((LOADS, dh, width), F32),
            pltpu.VMEM((n, 2, CHUNKS, ch, cols), BF16),
            pltpu.VMEM((2, 2, CHUNKS, ch, cols), BF16),
            pltpu.VMEM((n - 1, 2, CHUNKS, ch, cols), BF16),
            pltpu.VMEM((n, DOWN_CHUNKS, dh, width), BF16),
            dma((2 * LOADS,)),
            dma((n, 2, CHUNKS)),
            dma((n, 2, CHUNKS)),
            dma((2, 2, CHUNKS)),
            dma((2, CHUNKS)),
            dma((n, 2, CHUNKS)),
            dma((n, 2, CHUNKS)),
            dma((n, 2, CHUNKS)),
            dma((n, 2, CHUNKS)),
            dma((n, DOWN_CHUNKS)),
            dma((n, DOWN_CHUNKS)),
        ],
        name="move_weights",
        compiler_params=pltpu.CompilerParams(
            collective_id=0, has_side_effects=True, vmem_limit_bytes=56 << 20
        ),
    )(gain.reshape(rows, 1), w_gate, w_up, w_down)


def mix_kernel(rows_ref, weight_ref, gate_ref, up_ref, down_ref, gate_out, up_out, down_out, term_ref, total):
    j = pl.program_id(0)

    @pl.when(j == 0)
    def _():
        total[...] = jnp.zeros_like(total)

    gate, up, down = gate_ref[...], up_ref[...], down_ref[...]
    gate_out[...], up_out[...], down_out[...] = gate, up, down
    x = rows_ref[...]
    gate_act = jnp.dot(x, gate, preferred_element_type=F32)
    up_act = jnp.dot(x, up, preferred_element_type=F32)
    scale = weight_ref[:, :1].astype(F32)
    hidden = (gate_act / (1.0 + jnp.exp(-gate_act)) * up_act * scale).astype(BF16)
    total[...] += jnp.dot(hidden, down, preferred_element_type=F32)

    @pl.when(j == pl.num_programs(0) - 1)
    def _():
        term_ref[...] = total[...].astype(BF16)


def mix(packed, depth, gate, up, down):
    count = packed.shape[0]
    cols = gate.shape[1]
    wide = down.shape[1]
    tile = next(w for w in (256, 128) if cols % w == 0)
    whole = pl.BlockSpec((count, depth), lambda j: (0, 0))
    column = pl.BlockSpec((depth, tile), lambda j: (0, j))
    row = pl.BlockSpec((tile, wide), lambda j: (j, 0))
    return pl.pallas_call(
        mix_kernel,
        grid=(cols // tile,),
        out_shape=(
            jax.ShapeDtypeStruct(gate.shape, BF16),
            jax.ShapeDtypeStruct(up.shape, BF16),
            jax.ShapeDtypeStruct(down.shape, BF16),
            jax.ShapeDtypeStruct((count, wide), BF16),
        ),
        in_specs=[whole, pl.BlockSpec((count, 128), lambda j: (0, depth // 128)), column, column, row],
        out_specs=(column, column, row, pl.BlockSpec((count, wide), lambda j: (0, 0))),
        scratch_shapes=[pltpu.VMEM((count, wide), F32)],
        name="mix_tokens",
        compiler_params=pltpu.CompilerParams(vmem_limit_bytes=48 << 20),
    )(packed, packed, gate, up, down)


def sum_kernel(n, term_ref, out_ref, near, near_in, far, far_in, last, last_in, s1, r1, s2, r2, s3, r3):
    g, f, t = lax.axis_index("grp"), lax.axis_index("fs"), lax.axis_index("tp")
    mesh_id = pl.DeviceIdType.MESH
    width = out_ref.shape[1]
    count = out_ref.shape[0]
    mate = t + 1 - 2 * lax.rem(t, 2)
    over = lax.rem(t + 2, n)
    mate_over = lax.rem(mate + 2, n)

    barrier = pltpu.get_barrier_semaphore()
    for e in (mate, over):
        pl.semaphore_signal(barrier, inc=1, device_id=(g, f, e), device_id_type=mesh_id)
    for d in range(1, n):
        pl.semaphore_signal(barrier, inc=1, device_id=(g, lax.rem(f + d, n), t), device_id_type=mesh_id)
    pl.semaphore_wait(barrier, n + 1)

    def block(layer, column):
        return term_ref.at[pl.ds(pl.multiple_of(layer * count, count), count), pl.ds(pl.multiple_of(column * width, width), width)]

    def remote(src, dst, ssem, rsem, where):
        return pltpu.make_async_remote_copy(
            src_ref=src, dst_ref=dst, send_sem=ssem, recv_sem=rsem, device_id=where, device_id_type=mesh_id
        )

    layers = [lax.rem(f + d, n) for d in (2, 1, 3, 0)]

    def to_mate(i, h):
        column = mate_over if h == 0 else mate
        return remote(block(layers[i], column), near_in.at[h, i], s1.at[h, i], r1.at[h, i], (g, f, mate))

    def to_over(i):
        return remote(far.at[i], far_in.at[i], s2.at[i], r2.at[i], (g, f, over))

    def to_layer(i):
        return remote(last.at[i], last_in.at[f], s3.at[i], r3.at[f], (g, layers[i], t))

    def from_layer(layer):
        return remote(last.at[0], last_in.at[layer], s3.at[0], r3.at[layer], (g, layer, t))

    for i in range(n):
        for h in range(2):
            to_mate(i, h).start()
    for i in range(n):
        to_mate(i, 0).wait_recv()
        far[i] = (block(layers[i], over)[...].astype(F32) + near_in[0, i].astype(F32)).astype(BF16)
        to_mate(i, 1).wait_recv()
        near[i] = block(layers[i], t)[...].astype(F32) + near_in[1, i].astype(F32)
        to_over(i).start()
    for i in range(n):
        to_over(i).wait_recv()
        near[i] = near[i] + far_in[i].astype(F32)
        if i < n - 1:
            last[i] = near[i].astype(BF16)
            to_layer(i).start()
    total = near[n - 1]
    for d in range(1, n):
        layer = lax.rem(f + d, n)
        from_layer(layer).wait_recv()
        total = total + last_in[layer].astype(F32)
    out_ref[...] = total.astype(BF16)
    for i in range(n):
        for h in range(2):
            to_mate(i, h).wait_send()
        to_over(i).wait_send()
        if i < n - 1:
            to_layer(i).wait_send()


def sum_terms(n, term):
    count, width = term.shape[0] // n, term.shape[1] // n
    dma = pltpu.SemaphoreType.DMA
    vmem = pl.BlockSpec(memory_space=pltpu.VMEM)
    piece = (count, width)
    return pl.pallas_call(
        functools.partial(sum_kernel, n),
        out_shape=jax.ShapeDtypeStruct(piece, BF16),
        in_specs=[vmem],
        out_specs=vmem,
        scratch_shapes=[
            pltpu.VMEM((n, *piece), F32),
            pltpu.VMEM((2, n, *piece), BF16),
            pltpu.VMEM((n, *piece), BF16),
            pltpu.VMEM((n, *piece), BF16),
            pltpu.VMEM((n, *piece), BF16),
            pltpu.VMEM((n, *piece), BF16),
            dma((2, n)), dma((2, n)), dma((n,)), dma((n,)), dma((n,)), dma((n,)),
        ],
        name="sum_terms",
        compiler_params=pltpu.CompilerParams(collective_id=1, has_side_effects=True),
    )(term)


def fits(mesh, tokens, w_gate, w_down):
    groups, n, tp = mesh.shape["grp"], mesh.shape["fs"], mesh.shape["tp"]
    rows, cols = w_gate.shape[1:]
    hidden, width = w_down.shape[1:]
    return (
        groups == 2 and n == 4 and tp == 4 and w_gate.shape[0] == tp
        and cols == hidden and cols % 128 == 0 and width % 128 == 0 and tokens.shape[0] % 16 == 0
        and rows % (groups * CHUNKS * 16) == 0 and hidden % (DOWN_CHUNKS * 16) == 0
        and tokens.shape[0] * n <= 512
    )


def body(mesh, tokens, routes, route_logits, gain, w_gate, w_up, w_down):
    values = tokens.astype(F32)
    mean_square = jnp.mean(values * values, axis=-1, keepdims=True)
    normed = (values * lax.rsqrt(mean_square + 1e-06)).astype(BF16)
    expert_id = lax.axis_index("tp")
    first = jax.nn.sigmoid(route_logits[:, 0] - route_logits[:, 1])
    second = jax.nn.sigmoid(route_logits[:, 1] - route_logits[:, 0])
    weight_col = first * (routes[:, 0] == expert_id).astype(F32)
    weight_col = (weight_col + second * (routes[:, 1] == expert_id).astype(F32)).astype(BF16)
    packed = jnp.concatenate([normed, jnp.broadcast_to(weight_col[:, None], (normed.shape[0], 128))], axis=1)
    packed = lax.all_gather(packed, "fs", axis=0, tiled=True)
    n, depth = mesh.shape["fs"], normed.shape[1]
    if fits(mesh, tokens, w_gate, w_down):
        gate, up, down = move(mesh.shape["grp"], n, gain, w_gate, w_up, w_down)
        gate, up, down, term = mix(packed, depth, gate, up, down)
        return gate[None], up[None], down[None], sum_terms(n, term)
    gate = (w_gate * gain[None, :, None]).astype(BF16)
    up = (w_up * gain[None, :, None]).astype(BF16)
    spread = functools.partial(lax.all_to_all, axis_name="tp", split_axis=0, concat_axis=2, tiled=True)
    gate, up, down = spread(gate), spread(up), spread(w_down.astype(BF16))
    stack = functools.partial(lax.all_to_all, axis_name="fs", split_axis=2, concat_axis=1, tiled=True)
    gate, up = stack(gate), stack(up)
    rows, weight = packed[:, :depth], packed[:, depth : depth + 1]
    gate_act = jnp.dot(rows, gate[0], preferred_element_type=F32)
    up_act = jnp.dot(rows, up[0], preferred_element_type=F32)
    hidden = (jax.nn.silu(gate_act) * up_act * weight.astype(F32)).astype(BF16)
    term = jnp.dot(hidden, down[0], preferred_element_type=F32)
    by_feature = lax.psum_scatter(term, "tp", scatter_dimension=1, tiled=True)
    mixed = lax.psum_scatter(by_feature, "fs", scatter_dimension=0, tiled=True)
    return gate, up, down, mixed.astype(BF16)


def solution(mesh):
    return jax.shard_map(
        functools.partial(body, mesh),
        mesh=mesh,
        in_specs=(
            P(("grp", "fs"), None),
            P(("grp", "fs"), None),
            P(("grp", "fs"), None),
            P("fs"),
            P(None, "fs", "tp"),
            P(None, "fs", "tp"),
            P(None, "fs", "tp"),
        ),
        out_specs=(
            P(("grp", "tp"), None, "fs"),
            P(("grp", "tp"), None, "fs"),
            P(("grp", "tp"), "fs", None),
            P(("grp", "fs"), "tp"),
        ),
        check_vma=False,
    )
```

```python
import functools

import jax
import jax.numpy as jnp
from jax import lax
from jax.experimental import pallas as pl
from jax.experimental.pallas import tpu as pltpu
from jax.sharding import PartitionSpec as P

BF16 = jnp.bfloat16
F32 = jnp.float32
CHUNKS = 4
DOWN_CHUNKS = 4
LAGS = (2, 3, 4)
LOADS = 4


def move_kernel(
    groups, n, gain_ref, wg_ref, wu_ref, wd_ref, og_ref, ou_ref, od_ref,
    wide, wide_d, stage, extra, relay, stage_d,
    load_sem, s1s, s1r, xs, xr, zs, zr, ys, yr, ds, dr,
):
    g, f, t = lax.axis_index("grp"), lax.axis_index("fs"), lax.axis_index("tp")
    rows = wg_ref.shape[1]
    half = rows // groups
    ch = half // CHUNKS
    hidden, width = wd_ref.shape[1:]
    dh = hidden // DOWN_CHUNKS
    weights, outs = (wg_ref, wu_ref), (og_ref, ou_ref)
    items = 2 * CHUNKS

    mate = t + 1 - 2 * lax.rem(t, 2)
    peers = (t, mate, lax.rem(t + 2, n), lax.rem(mate + 2, n))
    home = f == t

    def remote(src, dst, ssem, rsem, where):
        return pltpu.make_async_remote_copy(
            src_ref=src, dst_ref=dst, send_sem=ssem, recv_sem=rsem,
            device_id=where, device_id_type=pl.DeviceIdType.MESH,
        )

    barrier = pltpu.get_barrier_semaphore()
    for k in (1, 2, 3):
        pl.semaphore_signal(barrier, inc=1, device_id=(g, f, peers[k]), device_id_type=pl.DeviceIdType.MESH)
    for d in range(1, n):
        pl.semaphore_signal(barrier, inc=1, device_id=(g, lax.rem(f + d, n), t), device_id_type=pl.DeviceIdType.MESH)
    pl.semaphore_signal(barrier, inc=1, device_id=(1 - g, f, t), device_id_type=pl.DeviceIdType.MESH)
    pl.semaphore_wait(barrier, 2 * n - 1)

    def own_row(c):
        return pl.multiple_of(g * half + c * ch, ch)

    def other_row(c):
        return pl.multiple_of((1 - g) * half + c * ch, ch)

    def at_rows(u, source, row):
        return outs[u].at[pl.ds(pl.multiple_of(source * rows + row, ch), ch), :]

    def first(k, u, c):
        return remote(stage.at[k, u, c], relay.at[k - 1, u, c], s1s.at[k, u, c], s1r.at[k, u, c], (g, f, peers[k]))

    def first_home(k, u, c):
        return remote(stage.at[k, u, c], at_rows(u, f, own_row(c)), s1s.at[k, u, c], s1r.at[k, u, c], (g, f, peers[k]))

    def own_home(u, c):
        return pltpu.make_async_copy(stage.at[0, u, c], at_rows(u, f, own_row(c)), s1s.at[0, u, c])

    def extra_home(u, c):
        return pltpu.make_async_copy(extra.at[0, u, c], at_rows(u, f, other_row(c)), xs.at[0, u, c])

    def extra_mate(u, c):
        return remote(extra.at[1, u, c], at_rows(u, f, other_row(c)), xs.at[1, u, c], xr.at[u, c], (g, f, mate))

    def layer(k, u, c):
        src = stage.at[0, u, c] if k == 0 else relay.at[k - 1, u, c]
        return remote(src, at_rows(u, f, own_row(c)), zs.at[k, u, c], zr.at[f, u, c], (g, peers[k], t))

    def layer_in(source, u, c):
        piece = at_rows(u, source, own_row(c))
        return remote(piece, piece, zs.at[0, u, c], zr.at[source, u, c], (1 - g, f, t))

    def across(source, u, c):
        piece = at_rows(u, source, own_row(c))
        return remote(piece, piece, ys.at[source, u, c], yr.at[source, u, c], (1 - g, f, t))

    def down(k, c):
        src = stage_d.at[k, c]
        dst = od_ref.at[pl.ds(c * dh, dh), pl.ds(pl.multiple_of(t * width, 128), width)]
        if k == 0:
            return pltpu.make_async_copy(src, dst, ds.at[0, c])
        return remote(src, dst, ds.at[k, c], dr.at[k, c], (g, f, peers[k]))

    order = (2, 0, 3, 1)

    def load(u, k, row, slot):
        return pltpu.make_async_copy(weights[u].at[peers[k], pl.ds(row, ch), :], wide.at[slot], load_sem.at[slot])

    def load_d(k, c, slot):
        return pltpu.make_async_copy(wd_ref.at[peers[k], pl.ds(c * dh, dh), :], wide_d.at[slot], load_sem.at[LOADS + slot])

    def fold(slot, row, dst):
        scale = gain_ref[pl.ds(row, ch), :]
        dst[...] = (wide[slot] * scale).astype(BF16)

    for j, k in enumerate(order):
        load(0, k, own_row(0), j).start()
    for u in range(2):
        def trip(c, _, u=u):
            for j, k in enumerate(order):
                load(u, k, own_row(c), j).wait()
                fold(j, own_row(c), stage.at[k, u, c])

                @pl.when(c < CHUNKS - 1)
                def _():
                    load(u, k, own_row(c + 1), j).start()

                if u == 0:
                    @pl.when(c == CHUNKS - 1)
                    def _():
                        load(1, k, own_row(0), j).start()

                if k == 0:
                    @pl.when(home)
                    def _():
                        own_home(u, c).start()

                    @pl.when(jnp.logical_not(home))
                    def _():
                        layer(0, u, c).start()
                else:
                    @pl.when(home)
                    def _():
                        first_home(k, u, c).start()

                    @pl.when(jnp.logical_not(home))
                    def _():
                        first(k, u, c).start()
            return 0

        lax.fori_loop(0, CHUNKS, trip, 0)

    for j, k in enumerate(order):
        load_d(k, 0, j).start()

    def trip_d(c, _):
        for j, k in enumerate(order):
            load_d(k, c, j).wait()
            stage_d[k, c] = wide_d[j].astype(BF16)

            @pl.when(c < DOWN_CHUNKS - 1)
            def _():
                load_d(k, c + 1, j).start()

            down(k, c).start()
        return 0

    lax.fori_loop(0, DOWN_CHUNKS, trip_d, 0)

    @pl.when(home)
    def _():
        for u in range(2):
            def trip_x(c, _, u=u):
                for k in (0, 1):
                    copy = load(u, k, other_row(c), k)
                    copy.start()
                    copy.wait()
                    fold(k, other_row(c), extra.at[k, u, c])
                    (extra_home if k == 0 else extra_mate)(u, c).start()
                return 0

            lax.fori_loop(0, CHUNKS, trip_x, 0)

    def forward_z(k, u, c):
        away = peers[k] != f

        @pl.when(away)
        def _():
            first(k, u, c).wait_recv()
            layer(k, u, c).start()

        @pl.when(jnp.logical_not(away))
        def _():
            first_home(k, u, c).wait_recv()
            if k >= 2:
                across(f, u, c).start()

    def forward_y(d, u, c):
        for sign in (1, -1):
            source = f + sign * d

            @pl.when((source >= 0) & (source < n))
            def _():
                layer_in(source, u, c).wait_recv()
                across(source, u, c).start()

    def at_item(fn, i):
        u, c = i // CHUNKS, lax.rem(i, CHUNKS)
        for v in range(2):
            @pl.when(u == v)
            def _():
                fn(v, c)

    def trip_f(i, _):
        def z_part(u, c):
            for k in (1, 2, 3):
                forward_z(k, u, c)

        @pl.when(i < items)
        def _():
            at_item(z_part, i)

        for d in range(1, n):
            lag = LAGS[d - 1]

            @pl.when((i >= lag) & (i < items + lag))
            def _():
                at_item(functools.partial(forward_y, d), i - lag)

        return 0

    lax.fori_loop(0, items + max(LAGS), trip_f, 0)

    for u in range(2):
        def trip_w(c, _, u=u):
            @pl.when(home)
            def _():
                own_home(u, c).wait()
                extra_home(u, c).wait()
                extra_mate(u, c).wait_send()

            @pl.when(jnp.logical_not(home))
            def _():
                layer(0, u, c).wait_send()

            @pl.when(f == mate)
            def _():
                extra_mate(u, c).wait_recv()

            for k in (1, 2, 3):
                first(k, u, c).wait_send()

                @pl.when(peers[k] != f)
                def _():
                    layer(k, u, c).wait_send()

                if k >= 2:
                    @pl.when(peers[k] == f)
                    def _():
                        across(f, u, c).wait()

            for d in range(1, n):
                for sign in (1, -1):
                    source = f + sign * d

                    @pl.when((source >= 0) & (source < n))
                    def _():
                        across(source, u, c).wait()
            return 0

        lax.fori_loop(0, CHUNKS, trip_w, 0)

    def trip_wd(c, _):
        for k in range(n):
            down(k, c).wait()
        return 0

    lax.fori_loop(0, DOWN_CHUNKS, trip_wd, 0)


def move(groups, n, gain, w_gate, w_up, w_down):
    experts, rows, cols = w_gate.shape
    hidden, width = w_down.shape[1:]
    ch = rows // groups // CHUNKS
    dh = hidden // DOWN_CHUNKS
    dma = pltpu.SemaphoreType.DMA
    hbm = pl.BlockSpec(memory_space=pl.ANY)
    return pl.pallas_call(
        functools.partial(move_kernel, groups, n),
        out_shape=(
            jax.ShapeDtypeStruct((rows * n, cols), BF16),
            jax.ShapeDtypeStruct((rows * n, cols), BF16),
            jax.ShapeDtypeStruct((hidden, width * n), BF16),
        ),
        in_specs=[pl.BlockSpec(memory_space=pltpu.VMEM), hbm, hbm, hbm],
        out_specs=(hbm, hbm, hbm),
        scratch_shapes=[
            pltpu.VMEM((LOADS, ch, cols), F32),
            pltpu.VMEM((LOADS, dh, width), F32),
            pltpu.VMEM((n, 2, CHUNKS, ch, cols), BF16),
            pltpu.VMEM((2, 2, CHUNKS, ch, cols), BF16),
            pltpu.VMEM((n - 1, 2, CHUNKS, ch, cols), BF16),
            pltpu.VMEM((n, DOWN_CHUNKS, dh, width), BF16),
            dma((2 * LOADS,)),
            dma((n, 2, CHUNKS)),
            dma((n, 2, CHUNKS)),
            dma((2, 2, CHUNKS)),
            dma((2, CHUNKS)),
            dma((n, 2, CHUNKS)),
            dma((n, 2, CHUNKS)),
            dma((n, 2, CHUNKS)),
            dma((n, 2, CHUNKS)),
            dma((n, DOWN_CHUNKS)),
            dma((n, DOWN_CHUNKS)),
        ],
        name="move_weights",
        compiler_params=pltpu.CompilerParams(
            collective_id=0, has_side_effects=True, vmem_limit_bytes=56 << 20
        ),
    )(gain.reshape(rows, 1), w_gate, w_up, w_down)


def mix_kernel(rows_ref, weight_ref, gate_ref, up_ref, down_ref, gate_out, up_out, down_out, term_ref, total):
    j = pl.program_id(0)

    @pl.when(j == 0)
    def _():
        total[...] = jnp.zeros_like(total)

    gate, up, down = gate_ref[...], up_ref[...], down_ref[...]
    gate_out[...], up_out[...], down_out[...] = gate, up, down
    x = rows_ref[...]
    gate_act = jnp.dot(x, gate, preferred_element_type=F32)
    up_act = jnp.dot(x, up, preferred_element_type=F32)
    scale = weight_ref[:, :1].astype(F32)
    hidden = (gate_act / (1.0 + jnp.exp(-gate_act)) * up_act * scale).astype(BF16)
    total[...] += jnp.dot(hidden, down, preferred_element_type=F32)

    @pl.when(j == pl.num_programs(0) - 1)
    def _():
        term_ref[...] = total[...].astype(BF16)


def mix(packed, depth, gate, up, down):
    count = packed.shape[0]
    cols = gate.shape[1]
    wide = down.shape[1]
    tile = next(w for w in (256, 128) if cols % w == 0)
    whole = pl.BlockSpec((count, depth), lambda j: (0, 0))
    column = pl.BlockSpec((depth, tile), lambda j: (0, j))
    row = pl.BlockSpec((tile, wide), lambda j: (j, 0))
    return pl.pallas_call(
        mix_kernel,
        grid=(cols // tile,),
        out_shape=(
            jax.ShapeDtypeStruct(gate.shape, BF16),
            jax.ShapeDtypeStruct(up.shape, BF16),
            jax.ShapeDtypeStruct(down.shape, BF16),
            jax.ShapeDtypeStruct((count, wide), BF16),
        ),
        in_specs=[whole, pl.BlockSpec((count, 128), lambda j: (0, depth // 128)), column, column, row],
        out_specs=(column, column, row, pl.BlockSpec((count, wide), lambda j: (0, 0))),
        scratch_shapes=[pltpu.VMEM((count, wide), F32)],
        name="mix_tokens",
        compiler_params=pltpu.CompilerParams(vmem_limit_bytes=48 << 20),
    )(packed, packed, gate, up, down)


def sum_kernel(n, term_ref, out_ref, near, near_in, far, far_in, last, last_in, s1, r1, s2, r2, s3, r3):
    g, f, t = lax.axis_index("grp"), lax.axis_index("fs"), lax.axis_index("tp")
    mesh_id = pl.DeviceIdType.MESH
    width = out_ref.shape[1]
    count = out_ref.shape[0]
    mate = t + 1 - 2 * lax.rem(t, 2)
    over = lax.rem(t + 2, n)
    mate_over = lax.rem(mate + 2, n)

    barrier = pltpu.get_barrier_semaphore()
    for e in (mate, over):
        pl.semaphore_signal(barrier, inc=1, device_id=(g, f, e), device_id_type=mesh_id)
    for d in range(1, n):
        pl.semaphore_signal(barrier, inc=1, device_id=(g, lax.rem(f + d, n), t), device_id_type=mesh_id)
    pl.semaphore_wait(barrier, n + 1)

    def block(layer, column):
        return term_ref.at[pl.ds(pl.multiple_of(layer * count, count), count), pl.ds(pl.multiple_of(column * width, width), width)]

    def remote(src, dst, ssem, rsem, where):
        return pltpu.make_async_remote_copy(
            src_ref=src, dst_ref=dst, send_sem=ssem, recv_sem=rsem, device_id=where, device_id_type=mesh_id
        )

    layers = [lax.rem(f + d, n) for d in (2, 1, 3, 0)]

    def to_mate(i, h):
        column = mate_over if h == 0 else mate
        return remote(block(layers[i], column), near_in.at[h, i], s1.at[h, i], r1.at[h, i], (g, f, mate))

    def to_over(i):
        return remote(far.at[i], far_in.at[i], s2.at[i], r2.at[i], (g, f, over))

    def to_layer(i):
        return remote(last.at[i], last_in.at[f], s3.at[i], r3.at[f], (g, layers[i], t))

    def from_layer(layer):
        return remote(last.at[0], last_in.at[layer], s3.at[0], r3.at[layer], (g, layer, t))

    for i in range(n):
        for h in range(2):
            to_mate(i, h).start()
    for i in range(n):
        to_mate(i, 0).wait_recv()
        far[i] = (block(layers[i], over)[...].astype(F32) + near_in[0, i].astype(F32)).astype(BF16)
        to_mate(i, 1).wait_recv()
        near[i] = block(layers[i], t)[...].astype(F32) + near_in[1, i].astype(F32)
        to_over(i).start()
    for i in range(n):
        to_over(i).wait_recv()
        near[i] = near[i] + far_in[i].astype(F32)
        if i < n - 1:
            last[i] = near[i].astype(BF16)
            to_layer(i).start()
    total = near[n - 1]
    for d in range(1, n):
        layer = lax.rem(f + d, n)
        from_layer(layer).wait_recv()
        total = total + last_in[layer].astype(F32)
    out_ref[...] = total.astype(BF16)
    for i in range(n):
        for h in range(2):
            to_mate(i, h).wait_send()
        to_over(i).wait_send()
        if i < n - 1:
            to_layer(i).wait_send()


def sum_terms(n, term):
    count, width = term.shape[0] // n, term.shape[1] // n
    dma = pltpu.SemaphoreType.DMA
    vmem = pl.BlockSpec(memory_space=pltpu.VMEM)
    piece = (count, width)
    return pl.pallas_call(
        functools.partial(sum_kernel, n),
        out_shape=jax.ShapeDtypeStruct(piece, BF16),
        in_specs=[vmem],
        out_specs=vmem,
        scratch_shapes=[
            pltpu.VMEM((n, *piece), F32),
            pltpu.VMEM((2, n, *piece), BF16),
            pltpu.VMEM((n, *piece), BF16),
            pltpu.VMEM((n, *piece), BF16),
            pltpu.VMEM((n, *piece), BF16),
            pltpu.VMEM((n, *piece), BF16),
            dma((2, n)), dma((2, n)), dma((n,)), dma((n,)), dma((n,)), dma((n,)),
        ],
        name="sum_terms",
        compiler_params=pltpu.CompilerParams(collective_id=1, has_side_effects=True),
    )(term)


def fits(mesh, tokens, w_gate, w_down):
    groups, n, tp = mesh.shape["grp"], mesh.shape["fs"], mesh.shape["tp"]
    rows, cols = w_gate.shape[1:]
    hidden, width = w_down.shape[1:]
    return (
        groups == 2 and n == 4 and tp == 4 and w_gate.shape[0] == tp
        and cols == hidden and cols % 128 == 0 and width % 128 == 0 and tokens.shape[0] % 16 == 0
        and rows % (groups * CHUNKS * 16) == 0 and hidden % (DOWN_CHUNKS * 16) == 0
        and tokens.shape[0] * n <= 512
    )


def body(mesh, tokens, routes, route_logits, gain, w_gate, w_up, w_down):
    values = tokens.astype(F32)
    mean_square = jnp.mean(values * values, axis=-1, keepdims=True)
    normed = (values * lax.rsqrt(mean_square + 1e-06)).astype(BF16)
    expert_id = lax.axis_index("tp")
    first = jax.nn.sigmoid(route_logits[:, 0] - route_logits[:, 1])
    second = jax.nn.sigmoid(route_logits[:, 1] - route_logits[:, 0])
    weight_col = first * (routes[:, 0] == expert_id).astype(F32)
    weight_col = (weight_col + second * (routes[:, 1] == expert_id).astype(F32)).astype(BF16)
    packed = jnp.concatenate([normed, jnp.broadcast_to(weight_col[:, None], (normed.shape[0], 128))], axis=1)
    packed = lax.all_gather(packed, "fs", axis=0, tiled=True)
    n, depth = mesh.shape["fs"], normed.shape[1]
    if fits(mesh, tokens, w_gate, w_down):
        gate, up, down = move(mesh.shape["grp"], n, gain, w_gate, w_up, w_down)
        gate, up, down, term = mix(packed, depth, gate, up, down)
        return gate[None], up[None], down[None], sum_terms(n, term)
    gate = (w_gate * gain[None, :, None]).astype(BF16)
    up = (w_up * gain[None, :, None]).astype(BF16)
    spread = functools.partial(lax.all_to_all, axis_name="tp", split_axis=0, concat_axis=2, tiled=True)
    gate, up, down = spread(gate), spread(up), spread(w_down.astype(BF16))
    stack = functools.partial(lax.all_to_all, axis_name="fs", split_axis=2, concat_axis=1, tiled=True)
    gate, up = stack(gate), stack(up)
    rows, weight = packed[:, :depth], packed[:, depth : depth + 1]
    gate_act = jnp.dot(rows, gate[0], preferred_element_type=F32)
    up_act = jnp.dot(rows, up[0], preferred_element_type=F32)
    hidden = (jax.nn.silu(gate_act) * up_act * weight.astype(F32)).astype(BF16)
    term = jnp.dot(hidden, down[0], preferred_element_type=F32)
    by_feature = lax.psum_scatter(term, "tp", scatter_dimension=1, tiled=True)
    mixed = lax.psum_scatter(by_feature, "fs", scatter_dimension=0, tiled=True)
    return gate, up, down, mixed.astype(BF16)


def solution(mesh):
    return jax.shard_map(
        functools.partial(body, mesh),
        mesh=mesh,
        in_specs=(
            P(("grp", "fs"), None),
            P(("grp", "fs"), None),
            P(("grp", "fs"), None),
            P("fs"),
            P(None, "fs", "tp"),
            P(None, "fs", "tp"),
            P(None, "fs", "tp"),
        ),
        out_specs=(
            P(("grp", "tp"), None, "fs"),
            P(("grp", "tp"), None, "fs"),
            P(("grp", "tp"), "fs", None),
            P(("grp", "fs"), "tp"),
        ),
        check_vma=False,
    )
```
